32 devices in a mesh: sp: 8 (over z, y), tp: 4 (over x, core).
Axes of the slice: x: 2, y: 2, z: 4, core: 2. Of those that a mesh axis runs over, the one named last changes fastest.
Arguments:
- tokens: bfloat16 [1024, 2048], P('sp', 'tp'), may hold values from -28 to 28
- norm_gain: bfloat16 [1, 2048], P(None, 'tp'), may hold values from 0.099609375 to 1.8984375
- conv_b_w: bfloat16 [2048, 1024], P(None, 'tp'), may hold values from -0.125 to 0.125
- conv_c_w: bfloat16 [2048, 1024], P(None, 'tp'), may hold values from -0.125 to 0.125
- conv_u_w: bfloat16 [2048, 1024], P(None, 'tp'), may hold values from -0.125 to 0.125
- conv_taps: bfloat16 [3, 1024], P(None, 'tp'), may hold values from -3.5 to 3.5
- query_w: bfloat16 [2048, 2048], P(None, 'tp'), may hold values from -0.125 to 0.125
- key_w: bfloat16 [2048, 2048], P(None, 'tp'), may hold values from -0.125 to 0.125
- value_w: bfloat16 [2048, 2048], P(None, 'tp'), may hold values from -0.125 to 0.125
- outgate_w: bfloat16 [2048, 2048], P(None, 'tp'), may hold values from -0.125 to 0.125
- gate_w: bfloat16 [2048, 2, 8], P(None, None, 'tp'), may hold values from -0.125 to 0.125
- gate_bias: float32 [2, 8], P(None, 'tp'), may hold values from -5 to 150
- mem_gain: bfloat16 [2048], P('tp'), may hold values from 0.099609375 to 1.8984375
- conv_out_w: bfloat16 [1024, 2048], P('tp'), may hold values from -0.1875 to 0.1875
- mem_out_w: bfloat16 [2048, 2048], P('tp'), may hold values from -0.125 to 0.125
Outputs:
- layer_out: bfloat16 [1024, 2048], P(('sp', 'tp'))
The draws below stay inside these ranges and needn't reach their ends.
All inputs are finite; a program needn't handle non-finite values.
Results may differ from the reference program's by a relative error of at most 0.014.
The reference program's roundings to bfloat16 on the way count: a program that leaves them out, or rounds other values in their place, can miss the bound.
Values may be sent and summed in bfloat16 or wider, within the bound.
A program may use at most 64 MiB of HBM per device.

```python
import math
import jax
import jax.numpy as jnp
from jax import lax

D = 2048
CONV = 1024
MHEADS = 8
HEAD_DIM = 256
KW = 3
BLOCK = 128
MDIM = 2048
TOKENS = 1024
N_TP = 4


def draw_tokens(key, part):
    keys = jax.random.split(key, 3)
    row_scale = jnp.exp(jax.random.uniform(keys[0], (TOKENS, 1), jnp.float32, math.log(0.3), math.log(3.0)))
    col_scale = jnp.linspace(0.6, 1.8, D, dtype=jnp.float32)[None, :]
    col_scale = col_scale * jax.random.uniform(keys[1], (1, D), jnp.float32, 0.8, 1.25)
    base = jnp.clip(jax.random.normal(keys[2], (TOKENS, D), jnp.float32), -4.0, 4.0)
    return (base * row_scale * col_scale).astype(jnp.bfloat16)


def draw_gate_bias(key, part):
    keys = jax.random.split(key, 5)
    order = jax.random.permutation(keys[0], MHEADS)
    fast = order < MHEADS // 2
    input_part = -2.0 + 0.8 * jnp.clip(jax.random.normal(keys[2], (MHEADS,), jnp.float32), -3.0, 3.0)
    quick = jax.random.uniform(keys[3], (MHEADS,), jnp.float32, 3.0, 4.0)
    slow = jax.random.uniform(keys[4], (MHEADS,), jnp.float32, 10.5, 12.0)
    forget_part = jnp.where(fast, quick, slow)
    return jnp.stack([input_part, forget_part]).astype(jnp.float32)


def block_levels(key, shape, cuts, low, top_value):
    level, own = 1.0, jax.random.fold_in(key, 6)
    for dim, shards_of in cuts:
        steps = jnp.exp(jax.random.uniform(jax.random.fold_in(own, dim), (shards_of,), jnp.float32, low / len(cuts), top_value / len(cuts)))
        level = level * jnp.repeat(steps, shape[dim] // shards_of).reshape([-1 if axis == dim else 1 for axis in range(len(shape))])
    return level


def bell_draw(rng, extent, spread, most, shards=(), kind=jnp.bfloat16):
    level = block_levels(rng, extent, shards, -0.22, 0.18) if shards else 1.0
    values = jax.random.normal(rng, extent, jnp.float32) * spread * level
    return jnp.minimum(jnp.maximum(values, -most), most).astype(kind)


def setup_inputs(seed: int = 0) -> dict:
    arg_keys = jax.random.split(jax.random.key(seed), 16)
    tokens = draw_tokens(jax.random.fold_in(arg_keys[15], 71), 0)
    norm_gain = jnp.clip(1.0 + 0.18 * jax.random.normal(arg_keys[1], (1, D), jnp.float32), 0.099609375, 1.8984375).astype(jnp.bfloat16)
    conv_b_w = bell_draw(arg_keys[2], (D, CONV), D ** -0.5, 0.125, ((1, 4),))
    conv_c_w = bell_draw(arg_keys[3], (D, CONV), D ** -0.5, 0.125, ((1, 4),))
    conv_u_w = bell_draw(arg_keys[4], (D, CONV), D ** -0.5, 0.125, ((1, 4),))
    conv_taps = bell_draw(arg_keys[5], (KW, CONV), KW ** -0.5, 3.5, ((1, 4),))
    query_w = bell_draw(arg_keys[6], (D, MDIM), D ** -0.5, 0.125, ((1, 4),))
    key_w = bell_draw(arg_keys[7], (D, MDIM), D ** -0.5, 0.125, ((1, 4),))
    value_w = bell_draw(arg_keys[8], (D, MDIM), D ** -0.5, 0.125, ((1, 4),))
    outgate_w = bell_draw(arg_keys[9], (D, MDIM), D ** -0.5, 0.125, ((1, 4),))
    gate_w = bell_draw(arg_keys[10], (D, 2, MHEADS), D ** -0.5, 0.125, ((2, 4),))
    gate_bias = draw_gate_bias(jax.random.fold_in(arg_keys[15], 71), 0)
    mem_gain = jnp.clip(1.0 + 0.18 * jax.random.normal(arg_keys[12], (MDIM,), jnp.float32), 0.099609375, 1.8984375).astype(jnp.bfloat16)
    conv_out_w = bell_draw(arg_keys[13], (CONV, D), CONV ** -0.5, 0.1875, ((0, 4),))
    mem_out_w = bell_draw(arg_keys[14], (MDIM, D), MDIM ** -0.5, 0.125, ((0, 4),))
    return dict(tokens=tokens, norm_gain=norm_gain, conv_b_w=conv_b_w, conv_c_w=conv_c_w, conv_u_w=conv_u_w, conv_taps=conv_taps, query_w=query_w, key_w=key_w, value_w=value_w, outgate_w=outgate_w, gate_w=gate_w, gate_bias=gate_bias, mem_gain=mem_gain, conv_out_w=conv_out_w, mem_out_w=mem_out_w)


EPS = 1e-06
HIGH = lax.Precision.HIGHEST

def block_step(carry, inputs):
    memory, normer, stabil = carry
    query_block, key_block, value_block, input_gate, log_forget = inputs
    length = query_block.shape[0]
    causal = jnp.tril(jnp.ones((length, length), dtype=bool))
    running = jnp.cumsum(log_forget)
    decays = jnp.where(causal, running[:, None] - running[None, :] + input_gate[None, :], -jnp.inf)
    inter = running + stabil
    row_max = jnp.maximum(inter, lax.optimization_barrier(jnp.max(decays, axis=1)))
    weights = jnp.exp(decays - row_max[:, None])
    scores = jnp.dot(query_block, key_block.T, precision=HIGH) * weights
    carried = jnp.exp(inter - row_max)
    numer_part = carried[:, None] * jnp.dot(query_block, memory, precision=HIGH) + jnp.dot(scores, value_block, precision=HIGH)
    denom_part = carried * jnp.dot(query_block, normer, precision=HIGH) + lax.optimization_barrier(jnp.sum(scores, axis=1))
    result = numer_part / jnp.maximum(jnp.abs(denom_part), jnp.exp(-row_max))[:, None]
    new_stabil = row_max[-1]
    key_weight = jnp.exp(running[-1] - running + input_gate - new_stabil)
    fade = jnp.exp(running[-1] + stabil - new_stabil)
    memory = fade * memory + jnp.dot((key_weight[:, None] * key_block).T, value_block, precision=HIGH)
    normer = fade * normer + jnp.dot(key_weight, key_block, precision=HIGH)
    return ((memory, normer, new_stabil), result)

def memory_head(queries, keys, values, input_pre, log_forget):
    count, width = queries.shape
    blocks = count // BLOCK
    inputs = (queries.reshape(blocks, BLOCK, width), keys.reshape(blocks, BLOCK, width), values.reshape(blocks, BLOCK, width), input_pre.reshape(blocks, BLOCK), log_forget.reshape(blocks, BLOCK))
    start = (jnp.zeros((width, width), jnp.float32), jnp.zeros((width,), jnp.float32), jnp.zeros((), jnp.float32))
    final, results = lax.scan(block_step, start, inputs)
    return results.reshape(count, width)

def reference(tokens, norm_gain, conv_b_w, conv_c_w, conv_u_w, conv_taps, query_w, key_w, value_w, outgate_w, gate_w, gate_bias, mem_gain, conv_out_w, mem_out_w):
    wide = tokens.astype(jnp.float32)
    inv_rms = lax.rsqrt(lax.optimization_barrier(jnp.mean(wide * wide, axis=1, keepdims=True)) + EPS)
    scaled = (wide * norm_gain.astype(jnp.float32)).astype(jnp.bfloat16)

    def project(weight):
        rounded = (inv_rms * jnp.dot(scaled, weight, preferred_element_type=jnp.float32)).astype(jnp.bfloat16)
        return lax.optimization_barrier(rounded).astype(jnp.float32)
    gate_b = project(conv_b_w)
    gate_c = project(conv_c_w)
    gate_u = project(conv_u_w)
    queries = project(query_w)
    keys = project(key_w)
    values = project(value_w)
    outgate = project(outgate_w)
    gates = inv_rms * jnp.dot(scaled, gate_w.reshape(D, 2 * MHEADS), preferred_element_type=jnp.float32)
    input_pre = gates[:, :MHEADS] + gate_bias[0]
    forget_pre = gates[:, MHEADS:] + gate_bias[1]
    mixed_in = lax.optimization_barrier((gate_c * gate_u).astype(jnp.bfloat16)).astype(jnp.float32)
    padded = jnp.concatenate([jnp.zeros((KW - 1, CONV), jnp.float32), mixed_in], axis=0)
    taps = conv_taps.astype(jnp.float32)
    conv_sum = jnp.zeros((TOKENS, CONV), jnp.float32)
    for offset in range(KW):
        conv_sum = conv_sum + taps[offset] * padded[offset:offset + TOKENS]
    y_conv = (gate_b * conv_sum).astype(jnp.bfloat16)
    head_q = queries.reshape(TOKENS, MHEADS, HEAD_DIM)
    head_k = keys.reshape(TOKENS, MHEADS, HEAD_DIM) * HEAD_DIM ** (-0.5)
    head_v = values.reshape(TOKENS, MHEADS, HEAD_DIM)
    mem_raw = jax.vmap(memory_head, in_axes=1, out_axes=1)(head_q, head_k, head_v, input_pre, jax.nn.log_sigmoid(forget_pre))
    flat_raw = mem_raw.reshape(TOKENS, MDIM)
    mem_norm = flat_raw * lax.rsqrt(lax.optimization_barrier(jnp.mean(flat_raw * flat_raw, axis=1, keepdims=True)) + EPS)
    mem_norm = mem_norm * mem_gain.astype(jnp.float32)[None, :]
    y_mem = (jax.nn.sigmoid(outgate) * mem_norm).astype(jnp.bfloat16)
    conv_width = CONV // N_TP
    mem_width = MDIM // N_TP
    total = jnp.zeros((TOKENS, D), jnp.float32)
    for group in range(N_TP):
        part = jnp.dot(y_conv[:, group * conv_width:(group + 1) * conv_width], conv_out_w[group * conv_width:(group + 1) * conv_width], preferred_element_type=jnp.float32)
        part = part + jnp.dot(y_mem[:, group * mem_width:(group + 1) * mem_width], mem_out_w[group * mem_width:(group + 1) * mem_width], preferred_element_type=jnp.float32)
        total = total + lax.optimization_barrier(part.astype(jnp.bfloat16)).astype(jnp.float32)
    return total.astype(jnp.bfloat16)
```

```python
import functools

import jax
import jax.numpy as jnp
from jax import lax
from jax.experimental import pallas as pl
from jax.experimental.pallas import tpu as pltpu
from jax.sharding import PartitionSpec as P

EPS = 1e-06
LOWEST = -1e30
HIGH = lax.Precision.HIGHEST
MESH = pl.DeviceIdType.MESH
F32 = jnp.float32
BF16 = jnp.bfloat16
GROUP = 128
NCHUNK = 4
NOUT = 4
EXTRA = 16


def dot(a, b, dims=((1,), (0,)), precision=None):
    return lax.dot_general(a, b, (dims, ((), ())), precision=precision, preferred_element_type=F32)


def kernel(n_sp, n_tp, heads, *refs):
    (tok, gain, wb, wc, wu, taps, wq, wk, wv, wo, gw, bias, mgain, cow, mow, out) = refs[:16]
    (
        full, scaled, vb, vc, vu, vq, vk, vv, vo, vg, vco, vmo,
        qs, ks, vs, og, own_c, got_a, got_p, put_p, in_c,
        meta, meta_a, meta_p, meta_s, meta_i, gates, gates_t,
        num, den, gb, mixed, halo, pad, yc, ym, sq_own, sq_got, part, rs,
        sem_w, sem_tok, tok_s, tok_r, a_s, a_r, p_s, p_r, h_s, h_r, q_s, q_r, r_s, r_r,
    ) = refs[16:]
    sp, tp = lax.axis_index("sp"), lax.axis_index("tp")
    count, feats = tok.shape
    model = n_tp * feats
    head_dim = wq.shape[1] // heads
    rows = head_dim // NCHUNK
    chips = n_tp // 2
    chip, core = tp // 2, lax.rem(tp, 2)
    mate = chip * 2 + 1 - core
    pair, odd = sp // 2, lax.rem(sp, 2)
    last_pair = n_sp // 2 - 1
    twin = sp + 1 - 2 * odd
    others = [lax.rem(tp + k, n_tp) for k in range(1, n_tp)]

    tok_copy = pltpu.make_async_copy(tok, full.at[tp, pl.ds(0, count)], sem_tok)
    tok_copy.start()
    loads = [
        pltpu.make_async_copy(src, dst, sem_w.at[i])
        for i, (src, dst) in enumerate(
            ((gw, vg), (wk, vk), (wv, vv), (wq, vq), (wc, vc), (wu, vu), (wb, vb), (wo, vo), (cow, vco), (mow, vmo))
        )
    ]
    for load in loads:
        load.start()
    wait_of = dict(zip(("g", "k", "v", "q", "c", "u", "b", "o", "co", "mo"), loads))
    full[tp, pl.ds(count, EXTRA), :] = jnp.broadcast_to(gain[...].astype(F32), (EXTRA, feats)).astype(BF16)

    barrier = pltpu.get_barrier_semaphore()
    steps = (1, -1, 2, -2)
    for other in others:
        pl.semaphore_signal(barrier, inc=1, device_id=(sp, other), device_id_type=MESH)
    for step in steps:
        @pl.when((sp + step >= 0) & (sp + step < n_sp))
        def _():
            pl.semaphore_signal(barrier, inc=1, device_id=(sp + step, tp), device_id_type=MESH)
    peers = n_tp - 1
    for step in steps:
        peers = peers + ((sp + step >= 0) & (sp + step < n_sp)).astype(jnp.int32)
    pl.semaphore_wait(barrier, peers)

    def send_tok(source, to, slot):
        copy = pltpu.make_async_remote_copy(
            src_ref=full.at[source], dst_ref=full.at[source], send_sem=tok_s.at[slot],
            recv_sem=tok_r.at[source], device_id=(sp, to), device_id_type=MESH)
        copy.start()
        return copy

    def got_tok(source):
        pltpu.make_async_remote_copy(
            src_ref=full.at[source], dst_ref=full.at[source], send_sem=tok_s.at[0],
            recv_sem=tok_r.at[source], device_id=(sp, mate), device_id_type=MESH).wait_recv()

    tok_copy.wait()
    tok_sends = []
    far = [lax.rem(chip + k, chips) for k in range(1, chips)]
    for k, x in enumerate(far):
        tok_sends.append(send_tok(tp, x * 2 + core, k))
    tok_sends.append(send_tok(tp, mate, chips - 1))
    for k, x in enumerate(far):
        got_tok(x * 2 + core)
        tok_sends.append(send_tok(x * 2 + core, mate, chips + k))
    got_tok(mate)
    for k, x in enumerate(far):
        got_tok(x * 2 + 1 - core)

    squares = jnp.zeros((count, 1), F32)
    for s in range(n_tp):
        wide = full[s, 0:count, :].astype(F32)
        scaled[:, s * feats:(s + 1) * feats] = (wide * full[s, count:count + 1, :].astype(F32)).astype(BF16)
        squares = squares + jnp.sum(wide * wide, axis=1, keepdims=True)
    inv = lax.rsqrt(squares / model + EPS)

    def project(ref, lo, hi):
        return (inv * dot(scaled[...], ref[:, lo:hi])).astype(BF16)

    wait_of["g"].wait()
    pre = inv * dot(scaled[...], vg[...], ((1,), (1,))) + bias[0:1, :]
    lf = jnp.minimum(pre, 0.0) - jnp.log1p(jnp.exp(-jnp.abs(pre)))
    row_id = lax.broadcasted_iota(jnp.int32, (count, count), 0)
    col_id = lax.broadcasted_iota(jnp.int32, (count, count), 1)
    causal = row_id >= col_id
    running = dot(causal.astype(F32), lf, precision=HIGH)
    lane = lax.broadcasted_iota(jnp.int32, (count, GROUP), 1)
    both = jnp.where(lane < heads, pre, running)
    gates[...] = both
    gates_t[...] = both.T

    def gate_parts(h):
        i_col, b_col = gates[:, h:h + 1], gates[:, heads + h:heads + h + 1]
        i_row, b_row = gates_t[h:h + 1, :], gates_t[heads + h:heads + h + 1, :]
        decays = jnp.where(causal, b_col - b_row + i_row, LOWEST)
        top = jnp.max(decays, axis=1, keepdims=True)
        return i_col, b_col, decays, top

    wait_of["k"].wait()
    wait_of["v"].wait()
    scale = head_dim ** -0.5
    a_sends = []

    def remote(src, dst, ss, rs_, to):
        return pltpu.make_async_remote_copy(
            src_ref=src, dst_ref=dst, send_sem=ss, recv_sem=rs_, device_id=to, device_id_type=MESH)

    for h in range(heads):
        lo, hi = h * head_dim, (h + 1) * head_dim
        ks[:, lo:hi] = project(vk, lo, hi)
        vs[:, lo:hi] = project(vv, lo, hi)
        i_col, b_col, _, top = gate_parts(h)
        total = b_col[count - 1:count, :]
        m_own = top[count - 1:count, :]
        weight = jnp.exp(total - b_col + i_col - m_own)
        wkeys = ks[:, lo:hi].astype(F32) * (weight * scale)
        meta[h, 0:1, :] = jnp.sum(wkeys, axis=0, keepdims=True)
        meta[h, 1:2, :] = jnp.broadcast_to(m_own, (1, head_dim))
        meta[h, 2:3, :] = jnp.broadcast_to(total, (1, head_dim))
        meta[h, 3:8, :] = jnp.zeros((5, head_dim), F32)
        own_c[h] = dot(wkeys.astype(BF16), vs[:, lo:hi], ((0,), (0,))).astype(BF16)
        copy = remote(meta.at[h], meta_a.at[h], a_s.at[h, NCHUNK], a_r.at[h, NCHUNK], (twin, tp))
        copy.start()
        a_sends.append(copy)
        for c in range(NCHUNK):
            at = pl.ds(c * rows, rows)
            copy = remote(own_c.at[h, at], got_a.at[h, at], a_s.at[h, c], a_r.at[h, c], (twin, tp))
            copy.start()
            a_sends.append(copy)

    wait_of["c"].wait()
    wait_of["u"].wait()
    conv = wc.shape[1]
    mix = (project(vc, 0, conv).astype(F32) * project(vu, 0, conv).astype(F32)).astype(BF16)
    mixed[...] = mix
    edge = remote(mixed.at[pl.ds(count - EXTRA, EXTRA)], halo, h_s, h_r, (sp + 1, tp))
    pl.when(sp < n_sp - 1)(edge.start)
    wait_of["q"].wait()
    for h in range(heads):
        qs[:, h * head_dim:(h + 1) * head_dim] = project(vq, h * head_dim, (h + 1) * head_dim)
    wait_of["b"].wait()
    gb[...] = project(vb, 0, conv)
    wait_of["o"].wait()
    for h in range(heads):
        og[:, h * head_dim:(h + 1) * head_dim] = project(vo, h * head_dim, (h + 1) * head_dim)

    def local_part():
        for h in range(heads):
            lo, hi = h * head_dim, (h + 1) * head_dim
            _, _, decays, top = gate_parts(h)
            scores = dot(qs[:, lo:hi], ks[:, lo:hi], ((1,), (1,))) * scale * jnp.exp(decays - top)
            den[h] = jnp.broadcast_to(jnp.sum(scores, axis=1, keepdims=True), (count, GROUP))
            num[h] = dot(scores.astype(BF16), vs[:, lo:hi])

        @pl.when(sp > 0)
        def _():
            edge.wait_recv()

        @pl.when(sp == 0)
        def _():
            halo[...] = jnp.zeros(halo.shape, BF16)
        pad[0:EXTRA, :] = halo[...].astype(F32)
        pad[EXTRA:EXTRA + count, :] = mixed[...].astype(F32)
        reach = taps.shape[0] - 1
        tap = taps[...].astype(F32)
        acc = tap[0:1, :] * pad[EXTRA - reach:EXTRA - reach + count, :]
        for j in range(1, reach + 1):
            acc = acc + tap[j:j + 1, :] * pad[EXTRA - reach + j:EXTRA - reach + j + count, :]
        yc[...] = (gb[...].astype(F32) * acc).astype(BF16)

    early = pair >= (last_pair + 1) // 2
    pl.when(early)(local_part)

    is_odd = odd == 1

    @pl.when(pair == 0)
    def _():
        for h in range(heads):
            got_p[h] = jnp.zeros((head_dim, head_dim), BF16)
            meta_p[h] = jnp.full((8, head_dim), 0.0, F32)
            meta_p[h, 1:2, :] = jnp.full((1, head_dim), LOWEST, F32)

    def chain(h, c):
        at = pl.ds(c * rows, rows)
        if c == NCHUNK:
            return remote(meta_s.at[h], meta_p.at[h], p_s.at[h, c], p_r.at[h, c], (sp + 2, tp))
        return remote(put_p.at[h, at], got_p.at[h, at], p_s.at[h, c], p_r.at[h, c], (sp + 2, tp))

    def pair_copy(h, c):
        return a_sends[h * (NCHUNK + 1) + (0 if c == NCHUNK else c + 1)]

    for h in range(heads):
        pair_copy(h, NCHUNK).wait_recv()
        pl.when(pair > 0)(chain(h, NCHUNK).wait_recv)
        own, got, before = meta[h], meta_a[h], meta_p[h]
        first = jnp.where(is_odd, got, own)
        second = jnp.where(is_odd, own, got)
        m_p, m_e, m_o = before[1:2, :], first[1:2, :], second[1:2, :]
        b_e, b_o = first[2:3, :], second[2:3, :]
        m_1 = jnp.maximum(b_e + m_p, m_e)
        m_2 = jnp.maximum(b_o + m_1, m_o)
        c_p = jnp.exp(b_o + (b_e + m_p) - m_2)
        c_e = jnp.exp(b_o + m_e - m_2)
        c_o = jnp.exp(m_o - m_2)
        meta_s[h] = jnp.zeros((8, head_dim), F32)
        meta_s[h, 0:1, :] = c_p * before[0:1, :] + c_e * first[0:1, :] + c_o * second[0:1, :]
        meta_s[h, 1:2, :] = m_2
        pl.when(pair < last_pair)(chain(h, NCHUNK).start)
        c_own = jnp.where(is_odd, c_o, c_e)
        c_got = jnp.where(is_odd, c_e, c_o)
        f_p = jnp.where(is_odd, jnp.exp(b_e + m_p - m_1), 1.0)
        f_e = jnp.where(is_odd, jnp.exp(m_e - m_1), 0.0)
        meta_in = (f_p * before[0:1, :] + f_e * first[0:1, :], jnp.where(is_odd, m_1, m_p))
        meta_i[h, 0:1, :] = meta_in[0]
        meta_i[h, 1:2, :] = meta_in[1]
        for c in range(NCHUNK):
            at = pl.ds(c * rows, rows)
            pair_copy(h, c).wait_recv()
            pl.when(pair > 0)(chain(h, c).wait_recv)
            block_p = got_p[h, at, :].astype(F32)
            block_a = got_a[h, at, :].astype(F32)
            put_p[h, at, :] = (c_p * block_p + c_own * own_c[h, at, :].astype(F32) + c_got * block_a).astype(BF16)
            pl.when(pair < last_pair)(chain(h, c).start)
            in_c[h, at, :] = (f_p * block_p + f_e * block_a).astype(BF16)

    pl.when(jnp.logical_not(early))(local_part)

    own_sq = jnp.zeros((count, 1), F32)
    for h in range(heads):
        lo, hi = h * head_dim, (h + 1) * head_dim
        _, b_col, _, top_own = gate_parts(h)
        n_in, m_in = meta_i[h, 0:1, :], meta_i[h, 1:2, 0:1]
        top = jnp.maximum(top_own, b_col + m_in)
        s_own = jnp.exp(top_own - top)
        s_in = jnp.exp(b_col + m_in - top)
        qh = qs[:, lo:hi]
        den_all = s_own * den[h, :, 0:1] + s_in * jnp.sum(qh.astype(F32) * n_in, axis=1, keepdims=True)
        num_all = s_own * num[h] + s_in * dot(qh, in_c[h])
        raw = num_all / jnp.maximum(jnp.abs(den_all), jnp.exp(-top))
        num[h] = raw
        own_sq = own_sq + jnp.sum(raw * raw, axis=1, keepdims=True)
    sq_own[...] = jnp.broadcast_to(own_sq, (count, GROUP)).T[0:8, :]
    sq_sends = []
    for k, other in enumerate(others):
        copy = remote(sq_own, sq_got.at[tp], q_s.at[k], q_r.at[tp], (sp, other))
        copy.start()
        sq_sends.append(copy)
    total_sq = sq_own[...]
    for k, other in enumerate(others):
        remote(sq_own, sq_got.at[other], q_s.at[k], q_r.at[other], (sp, other)).wait_recv()
        total_sq = total_sq + sq_got[other]
    features = n_tp * heads * head_dim
    norm_row = lax.rsqrt(total_sq[0:1, :] / features + EPS)
    norm = jnp.broadcast_to(norm_row, (count, count)).T[:, 0:1]
    for h in range(heads):
        lo, hi = h * head_dim, (h + 1) * head_dim
        normed = num[h] * norm * mgain[:, lo:hi].astype(F32)
        sig = 1.0 / (1.0 + jnp.exp(-og[:, lo:hi].astype(F32)))
        ym[:, lo:hi] = (sig * normed).astype(BF16)

    wait_of["co"].wait()
    wait_of["mo"].wait()
    share = count // n_tp
    width = model // NOUT
    out_sends = []
    for j in range(NOUT):
        at = pl.ds(j * width, width)
        part[:, j * width:(j + 1) * width] = (
            dot(yc[...], vco[:, j * width:(j + 1) * width]) + dot(ym[...], vmo[:, j * width:(j + 1) * width])
        ).astype(BF16)
        for k, other in enumerate(others):
            mine = pl.ds(pl.multiple_of(other * share, share), share)
            copy = remote(part.at[mine, at], rs.at[tp, :, at], r_s.at[j, k], r_r.at[j, tp], (sp, other))
            copy.start()
            out_sends.append(copy)
    mine = pl.ds(pl.multiple_of(tp * share, share), share)
    for j in range(NOUT):
        at = pl.ds(j * width, width)
        acc = part[mine, j * width:(j + 1) * width].astype(F32)
        for k, other in enumerate(others):
            remote(part.at[mine, at], rs.at[other, :, at], r_s.at[j, k], r_r.at[j, other], (sp, other)).wait_recv()
            acc = acc + rs[other, :, j * width:(j + 1) * width].astype(F32)
        out[:, j * width:(j + 1) * width] = acc.astype(BF16)

    for copy in tok_sends + a_sends + sq_sends + out_sends:
        copy.wait_send()
    pl.when(sp < n_sp - 1)(edge.wait_send)

    @pl.when(pair < last_pair)
    def _():
        for h in range(heads):
            for c in range(NCHUNK + 1):
                chain(h, c).wait_send()


def body(n_sp, n_tp, tokens, norm_gain, conv_b_w, conv_c_w, conv_u_w, conv_taps, query_w, key_w,
         value_w, outgate_w, gate_w, gate_bias, mem_gain, conv_out_w, mem_out_w):
    count, feats = tokens.shape
    model, conv = conv_b_w.shape
    mem = query_w.shape[1]
    heads = gate_bias.shape[1]
    head_dim = mem // heads
    share = count // n_tp
    gates_w = jnp.transpose(gate_w, (1, 2, 0)).reshape(2 * heads, model)
    gates_w = jnp.pad(gates_w, ((0, GROUP - 2 * heads), (0, 0)))
    bias = jnp.pad(gate_bias.reshape(1, 2 * heads), ((0, 0), (0, GROUP - 2 * heads)))
    vmem, hbm = pl.BlockSpec(memory_space=pltpu.VMEM), pl.BlockSpec(memory_space=pl.ANY)
    V, S = pltpu.VMEM, pltpu.SemaphoreType.DMA
    state = V((heads, head_dim, head_dim), BF16)
    small = V((heads, 8, head_dim), F32)
    scratch = [
        V((n_tp, count + EXTRA, feats), BF16), V((count, model), BF16),
        V((model, conv), BF16), V((model, conv), BF16), V((model, conv), BF16),
        V((model, mem), BF16), V((model, mem), BF16), V((model, mem), BF16), V((model, mem), BF16),
        V((GROUP, model), BF16), V((conv, model), BF16), V((mem, model), BF16),
        V((count, mem), BF16), V((count, mem), BF16), V((count, mem), BF16), V((count, mem), BF16),
        state, state, state, state, state,
        small, small, small, small, small, V((count, GROUP), F32), V((GROUP, count), F32),
        V((heads, count, head_dim), F32), V((heads, count, GROUP), F32),
        V((count, conv), BF16), V((count, conv), BF16), V((EXTRA, conv), BF16), V((count + EXTRA, conv), F32),
        V((count, conv), BF16), V((count, mem), BF16),
        V((8, count), F32), V((n_tp, 8, count), F32),
        V((count, model), BF16), V((n_tp, share, model), BF16),
        S((10,)), S, S((n_tp,)), S((n_tp,)),
        S((heads, NCHUNK + 1)), S((heads, NCHUNK + 1)), S((heads, NCHUNK + 1)), S((heads, NCHUNK + 1)),
        S, S, S((n_tp,)), S((n_tp,)), S((NOUT, n_tp)), S((NOUT, n_tp)),
    ]
    return pl.pallas_call(
        functools.partial(kernel, n_sp, n_tp, heads),
        out_shape=jax.ShapeDtypeStruct((share, model), BF16),
        in_specs=[hbm, vmem, hbm, hbm, hbm, vmem, hbm, hbm, hbm, hbm, hbm, vmem, vmem, hbm, hbm],
        out_specs=vmem,
        scratch_shapes=scratch,
        compiler_params=pltpu.CompilerParams(
            collective_id=0, has_side_effects=True, vmem_limit_bytes=60 * 1024 * 1024),
        name="mixer",
    )(tokens, norm_gain, conv_b_w, conv_c_w, conv_u_w, conv_taps, query_w, key_w, value_w, outgate_w,
      gates_w, bias, mem_gain.reshape(1, mem), conv_out_w, mem_out_w)


def solution(mesh):
    n_sp, n_tp = mesh.shape["sp"], mesh.shape["tp"]
    cols, rows = P(None, "tp"), P("tp", None)
    return jax.shard_map(
        functools.partial(body, n_sp, n_tp),
        mesh=mesh,
        in_specs=(
            P("sp", "tp"), cols, cols, cols, cols, cols, cols, cols, cols, cols,
            P(None, None, "tp"), cols, P("tp"), rows, rows,
        ),
        out_specs=P(("sp", "tp"), None),
        check_vma=False,
    )
```

```python
import functools

import jax
import jax.numpy as jnp
from jax import lax
from jax.experimental import pallas as pl
from jax.experimental.pallas import tpu as pltpu
from jax.sharding import PartitionSpec as P

EPS = 1e-06
LOWEST = -1e30
HIGH = lax.Precision.HIGHEST
MESH = pl.DeviceIdType.MESH
F32 = jnp.float32
BF16 = jnp.bfloat16
GROUP = 128
NCHUNK = 4
NOUT = 4
EXTRA = 16


def dot(a, b, dims=((1,), (0,)), precision=None):
    return lax.dot_general(a, b, (dims, ((), ())), precision=precision, preferred_element_type=F32)


def kernel(n_sp, n_tp, heads, *refs):
    (tok, gain, wb, wc, wu, taps, wq, wk, wv, wo, gw, bias, mgain, cow, mow, out) = refs[:16]
    (
        full, scaled, vb, vc, vu, vq, vk, vv, vo, vg, raw_g, raw_b, vco, vmo,
        qs, ks, vs, og, own_c, got_a, got_p, put_p, in_c,
        meta, meta_a, meta_p, meta_s, meta_i, gates, gates_t,
        num, den, gb, mixed, halo, pad, yc, ym, sq_own, sq_got, part, rs,
        sem_w, sem_tok, tok_s, tok_r, a_s, a_r, p_s, p_r, h_s, h_r, q_s, q_r, r_s, r_r,
    ) = refs[16:]
    sp, tp = lax.axis_index("sp"), lax.axis_index("tp")
    count, feats = tok.shape
    model = n_tp * feats
    head_dim = wq.shape[1] // heads
    rows = head_dim // NCHUNK
    chips = n_tp // 2
    chip, core = tp // 2, lax.rem(tp, 2)
    mate = chip * 2 + 1 - core
    pair, odd = sp // 2, lax.rem(sp, 2)
    last_pair = n_sp // 2 - 1
    twin = sp + 1 - 2 * odd
    others = [lax.rem(tp + k, n_tp) for k in range(1, n_tp)]

    tok_copy = pltpu.make_async_copy(tok, full.at[tp, pl.ds(0, count)], sem_tok)
    tok_copy.start()
    loads = [
        pltpu.make_async_copy(src, dst, sem_w.at[i])
        for i, (src, dst) in enumerate(
            ((wk, vk), (wv, vv), (wq, vq), (wc, vc), (wu, vu), (wb, vb), (wo, vo), (cow, vco), (mow, vmo))
        )
    ]
    for load in loads:
        load.start()
    wait_of = dict(zip(("k", "v", "q", "c", "u", "b", "o", "co", "mo"), loads))
    full[tp, pl.ds(count, EXTRA), :] = jnp.broadcast_to(gain[...].astype(F32), (EXTRA, feats)).astype(BF16)

    raw_g[...] = jnp.zeros(raw_g.shape, F32)
    raw_b[...] = jnp.zeros(raw_b.shape, F32)
    for i in range(2):
        raw_g[i * heads:(i + 1) * heads, :] = gw[i].astype(F32)
        raw_b[0:1, i * heads:(i + 1) * heads] = bias[i:i + 1, :]
    vg[0:EXTRA, :] = raw_g[...].astype(BF16)
    vg[EXTRA:GROUP, :] = jnp.zeros((GROUP - EXTRA, model), BF16)

    barrier = pltpu.get_barrier_semaphore()
    steps = (1, -1, 2, -2)
    for other in others:
        pl.semaphore_signal(barrier, inc=1, device_id=(sp, other), device_id_type=MESH)
    for step in steps:
        @pl.when((sp + step >= 0) & (sp + step < n_sp))
        def _():
            pl.semaphore_signal(barrier, inc=1, device_id=(sp + step, tp), device_id_type=MESH)
    peers = n_tp - 1
    for step in steps:
        peers = peers + ((sp + step >= 0) & (sp + step < n_sp)).astype(jnp.int32)
    pl.semaphore_wait(barrier, peers)

    def send_tok(source, to, slot):
        copy = pltpu.make_async_remote_copy(
            src_ref=full.at[source], dst_ref=full.at[source], send_sem=tok_s.at[slot],
            recv_sem=tok_r.at[source], device_id=(sp, to), device_id_type=MESH)
        copy.start()
        return copy

    def got_tok(source):
        pltpu.make_async_remote_copy(
            src_ref=full.at[source], dst_ref=full.at[source], send_sem=tok_s.at[0],
            recv_sem=tok_r.at[source], device_id=(sp, mate), device_id_type=MESH).wait_recv()

    tok_copy.wait()
    tok_sends = []
    far = [lax.rem(chip + k, chips) for k in range(1, chips)]
    for k, x in enumerate(far):
        tok_sends.append(send_tok(tp, x * 2 + core, k))
    tok_sends.append(send_tok(tp, mate, chips - 1))
    for k, x in enumerate(far):
        got_tok(x * 2 + core)
        tok_sends.append(send_tok(x * 2 + core, mate, chips + k))
    got_tok(mate)
    for k, x in enumerate(far):
        got_tok(x * 2 + 1 - core)

    squares = jnp.zeros((count, 1), F32)
    for s in range(n_tp):
        wide = full[s, 0:count, :].astype(F32)
        scaled[:, s * feats:(s + 1) * feats] = (wide * full[s, count:count + 1, :].astype(F32)).astype(BF16)
        squares = squares + jnp.sum(wide * wide, axis=1, keepdims=True)
    inv = lax.rsqrt(squares / model + EPS)

    def project(ref, lo, hi):
        return (inv * dot(scaled[...], ref[:, lo:hi])).astype(BF16)

    pre = inv * dot(scaled[...], vg[...], ((1,), (1,))) + raw_b[0:1, :]
    lf = jnp.minimum(pre, 0.0) - jnp.log1p(jnp.exp(-jnp.abs(pre)))
    row_id = lax.broadcasted_iota(jnp.int32, (count, count), 0)
    col_id = lax.broadcasted_iota(jnp.int32, (count, count), 1)
    causal = row_id >= col_id
    running = dot(causal.astype(F32), lf, precision=HIGH)
    lane = lax.broadcasted_iota(jnp.int32, (count, GROUP), 1)
    both = jnp.where(lane < heads, pre, running)
    gates[...] = both
    gates_t[...] = both.T

    def gate_parts(h):
        i_col, b_col = gates[:, h:h + 1], gates[:, heads + h:heads + h + 1]
        i_row, b_row = gates_t[h:h + 1, :], gates_t[heads + h:heads + h + 1, :]
        decays = jnp.where(causal, b_col - b_row + i_row, LOWEST)
        top = jnp.max(decays, axis=1, keepdims=True)
        return i_col, b_col, decays, top

    wait_of["k"].wait()
    wait_of["v"].wait()
    scale = head_dim ** -0.5
    a_sends = []

    def remote(src, dst, ss, rs_, to):
        return pltpu.make_async_remote_copy(
            src_ref=src, dst_ref=dst, send_sem=ss, recv_sem=rs_, device_id=to, device_id_type=MESH)

    for h in range(heads):
        lo, hi = h * head_dim, (h + 1) * head_dim
        ks[:, lo:hi] = project(vk, lo, hi)
        vs[:, lo:hi] = project(vv, lo, hi)
        i_col, b_col, _, top = gate_parts(h)
        total = b_col[count - 1:count, :]
        m_own = top[count - 1:count, :]
        weight = jnp.exp(total - b_col + i_col - m_own)
        wkeys = ks[:, lo:hi].astype(F32) * (weight * scale)
        meta[h, 0:1, :] = jnp.sum(wkeys, axis=0, keepdims=True)
        meta[h, 1:2, :] = jnp.broadcast_to(m_own, (1, head_dim))
        meta[h, 2:3, :] = jnp.broadcast_to(total, (1, head_dim))
        meta[h, 3:8, :] = jnp.zeros((5, head_dim), F32)
        own_c[h] = dot(wkeys.astype(BF16), vs[:, lo:hi], ((0,), (0,))).astype(BF16)
        copy = remote(meta.at[h], meta_a.at[h], a_s.at[h, NCHUNK], a_r.at[h, NCHUNK], (twin, tp))
        copy.start()
        a_sends.append(copy)
        for c in range(NCHUNK):
            at = pl.ds(c * rows, rows)
            copy = remote(own_c.at[h, at], got_a.at[h, at], a_s.at[h, c], a_r.at[h, c], (twin, tp))
            copy.start()
            a_sends.append(copy)

    wait_of["c"].wait()
    wait_of["u"].wait()
    conv = wc.shape[1]
    mix = (project(vc, 0, conv).astype(F32) * project(vu, 0, conv).astype(F32)).astype(BF16)
    mixed[...] = mix
    edge = remote(mixed.at[pl.ds(count - EXTRA, EXTRA)], halo, h_s, h_r, (sp + 1, tp))
    pl.when(sp < n_sp - 1)(edge.start)
    wait_of["q"].wait()
    for h in range(heads):
        qs[:, h * head_dim:(h + 1) * head_dim] = project(vq, h * head_dim, (h + 1) * head_dim)
    wait_of["b"].wait()
    gb[...] = project(vb, 0, conv)
    wait_of["o"].wait()
    for h in range(heads):
        og[:, h * head_dim:(h + 1) * head_dim] = project(vo, h * head_dim, (h + 1) * head_dim)

    def local_part():
        for h in range(heads):
            lo, hi = h * head_dim, (h + 1) * head_dim
            _, _, decays, top = gate_parts(h)
            scores = dot(qs[:, lo:hi], ks[:, lo:hi], ((1,), (1,))) * scale * jnp.exp(decays - top)
            den[h] = jnp.broadcast_to(jnp.sum(scores, axis=1, keepdims=True), (count, GROUP))
            num[h] = dot(scores.astype(BF16), vs[:, lo:hi])

        @pl.when(sp > 0)
        def _():
            edge.wait_recv()

        @pl.when(sp == 0)
        def _():
            halo[...] = jnp.zeros(halo.shape, BF16)
        pad[0:EXTRA, :] = halo[...].astype(F32)
        pad[EXTRA:EXTRA + count, :] = mixed[...].astype(F32)
        reach = taps.shape[0] - 1
        tap = taps[...].astype(F32)
        acc = tap[0:1, :] * pad[EXTRA - reach:EXTRA - reach + count, :]
        for j in range(1, reach + 1):
            acc = acc + tap[j:j + 1, :] * pad[EXTRA - reach + j:EXTRA - reach + j + count, :]
        yc[...] = (gb[...].astype(F32) * acc).astype(BF16)

    early = pair >= (last_pair + 1) // 2
    pl.when(early)(local_part)

    is_odd = odd == 1

    @pl.when(pair == 0)
    def _():
        for h in range(heads):
            got_p[h] = jnp.zeros((head_dim, head_dim), BF16)
            meta_p[h] = jnp.full((8, head_dim), 0.0, F32)
            meta_p[h, 1:2, :] = jnp.full((1, head_dim), LOWEST, F32)

    def chain(h, c):
        at = pl.ds(c * rows, rows)
        if c == NCHUNK:
            return remote(meta_s.at[h], meta_p.at[h], p_s.at[h, c], p_r.at[h, c], (sp + 2, tp))
        return remote(put_p.at[h, at], got_p.at[h, at], p_s.at[h, c], p_r.at[h, c], (sp + 2, tp))

    def pair_copy(h, c):
        return a_sends[h * (NCHUNK + 1) + (0 if c == NCHUNK else c + 1)]

    for h in range(heads):
        pair_copy(h, NCHUNK).wait_recv()
        pl.when(pair > 0)(chain(h, NCHUNK).wait_recv)
        own, got, before = meta[h], meta_a[h], meta_p[h]
        first = jnp.where(is_odd, got, own)
        second = jnp.where(is_odd, own, got)
        m_p, m_e, m_o = before[1:2, :], first[1:2, :], second[1:2, :]
        b_e, b_o = first[2:3, :], second[2:3, :]
        m_1 = jnp.maximum(b_e + m_p, m_e)
        m_2 = jnp.maximum(b_o + m_1, m_o)
        c_p = jnp.exp(b_o + (b_e + m_p) - m_2)
        c_e = jnp.exp(b_o + m_e - m_2)
        c_o = jnp.exp(m_o - m_2)
        meta_s[h] = jnp.zeros((8, head_dim), F32)
        meta_s[h, 0:1, :] = c_p * before[0:1, :] + c_e * first[0:1, :] + c_o * second[0:1, :]
        meta_s[h, 1:2, :] = m_2
        pl.when(pair < last_pair)(chain(h, NCHUNK).start)
        c_own = jnp.where(is_odd, c_o, c_e)
        c_got = jnp.where(is_odd, c_e, c_o)
        f_p = jnp.where(is_odd, jnp.exp(b_e + m_p - m_1), 1.0)
        f_e = jnp.where(is_odd, jnp.exp(m_e - m_1), 0.0)
        meta_in = (f_p * before[0:1, :] + f_e * first[0:1, :], jnp.where(is_odd, m_1, m_p))
        meta_i[h, 0:1, :] = meta_in[0]
        meta_i[h, 1:2, :] = meta_in[1]
        for c in range(NCHUNK):
            at = pl.ds(c * rows, rows)
            pair_copy(h, c).wait_recv()
            pl.when(pair > 0)(chain(h, c).wait_recv)
            block_p = got_p[h, at, :].astype(F32)
            block_a = got_a[h, at, :].astype(F32)
            put_p[h, at, :] = (c_p * block_p + c_own * own_c[h, at, :].astype(F32) + c_got * block_a).astype(BF16)
            pl.when(pair < last_pair)(chain(h, c).start)
            in_c[h, at, :] = (f_p * block_p + f_e * block_a).astype(BF16)

    pl.when(jnp.logical_not(early))(local_part)

    own_sq = jnp.zeros((count, 1), F32)
    for h in range(heads):
        lo, hi = h * head_dim, (h + 1) * head_dim
        _, b_col, _, top_own = gate_parts(h)
        n_in, m_in = meta_i[h, 0:1, :], meta_i[h, 1:2, 0:1]
        top = jnp.maximum(top_own, b_col + m_in)
        s_own = jnp.exp(top_own - top)
        s_in = jnp.exp(b_col + m_in - top)
        qh = qs[:, lo:hi]
        den_all = s_own * den[h, :, 0:1] + s_in * jnp.sum(qh.astype(F32) * n_in, axis=1, keepdims=True)
        num_all = s_own * num[h] + s_in * dot(qh, in_c[h])
        raw = num_all / jnp.maximum(jnp.abs(den_all), jnp.exp(-top))
        num[h] = raw
        own_sq = own_sq + jnp.sum(raw * raw, axis=1, keepdims=True)
    sq_own[...] = jnp.broadcast_to(own_sq, (count, GROUP)).T[0:8, :]
    sq_sends = []
    for k, other in enumerate(others):
        copy = remote(sq_own, sq_got.at[tp], q_s.at[k], q_r.at[tp], (sp, other))
        copy.start()
        sq_sends.append(copy)
    total_sq = sq_own[...]
    for k, other in enumerate(others):
        remote(sq_own, sq_got.at[other], q_s.at[k], q_r.at[other], (sp, other)).wait_recv()
        total_sq = total_sq + sq_got[other]
    features = n_tp * heads * head_dim
    norm_row = lax.rsqrt(total_sq[0:1, :] / features + EPS)
    norm = jnp.broadcast_to(norm_row, (count, count)).T[:, 0:1]
    for h in range(heads):
        lo, hi = h * head_dim, (h + 1) * head_dim
        normed = num[h] * norm * mgain[lo:hi].astype(F32).reshape(1, head_dim)
        sig = 1.0 / (1.0 + jnp.exp(-og[:, lo:hi].astype(F32)))
        ym[:, lo:hi] = (sig * normed).astype(BF16)

    wait_of["co"].wait()
    wait_of["mo"].wait()
    share = count // n_tp
    width = model // NOUT
    out_sends = []
    for j in range(NOUT):
        at = pl.ds(j * width, width)
        part[:, j * width:(j + 1) * width] = (
            dot(yc[...], vco[:, j * width:(j + 1) * width]) + dot(ym[...], vmo[:, j * width:(j + 1) * width])
        ).astype(BF16)
        for k, other in enumerate(others):
            mine = pl.ds(pl.multiple_of(other * share, share), share)
            copy = remote(part.at[mine, at], rs.at[tp, :, at], r_s.at[j, k], r_r.at[j, tp], (sp, other))
            copy.start()
            out_sends.append(copy)
    mine = pl.ds(pl.multiple_of(tp * share, share), share)
    for j in range(NOUT):
        at = pl.ds(j * width, width)
        acc = part[mine, j * width:(j + 1) * width].astype(F32)
        for k, other in enumerate(others):
            remote(part.at[mine, at], rs.at[other, :, at], r_s.at[j, k], r_r.at[j, other], (sp, other)).wait_recv()
            acc = acc + rs[other, :, j * width:(j + 1) * width].astype(F32)
        out[:, j * width:(j + 1) * width] = acc.astype(BF16)

    for copy in tok_sends + a_sends + sq_sends + out_sends:
        copy.wait_send()
    pl.when(sp < n_sp - 1)(edge.wait_send)

    @pl.when(pair < last_pair)
    def _():
        for h in range(heads):
            for c in range(NCHUNK + 1):
                chain(h, c).wait_send()


def body(n_sp, n_tp, tokens, norm_gain, conv_b_w, conv_c_w, conv_u_w, conv_taps, query_w, key_w,
         value_w, outgate_w, gate_w, gate_bias, mem_gain, conv_out_w, mem_out_w):
    count, feats = tokens.shape
    model, conv = conv_b_w.shape
    mem = query_w.shape[1]
    heads = gate_bias.shape[1]
    head_dim = mem // heads
    share = count // n_tp
    gates_w = jnp.transpose(gate_w, (1, 2, 0))
    vmem, hbm = pl.BlockSpec(memory_space=pltpu.VMEM), pl.BlockSpec(memory_space=pl.ANY)
    V, S = pltpu.VMEM, pltpu.SemaphoreType.DMA
    state = V((heads, head_dim, head_dim), BF16)
    small = V((heads, 8, head_dim), F32)
    scratch = [
        V((n_tp, count + EXTRA, feats), BF16), V((count, model), BF16),
        V((model, conv), BF16), V((model, conv), BF16), V((model, conv), BF16),
        V((model, mem), BF16), V((model, mem), BF16), V((model, mem), BF16), V((model, mem), BF16),
        V((GROUP, model), BF16), V((EXTRA, model), F32), V((8, GROUP), F32), V((conv, model), BF16), V((mem, model), BF16),
        V((count, mem), BF16), V((count, mem), BF16), V((count, mem), BF16), V((count, mem), BF16),
        state, state, state, state, state,
        small, small, small, small, small, V((count, GROUP), F32), V((GROUP, count), F32),
        V((heads, count, head_dim), F32), V((heads, count, GROUP), F32),
        V((count, conv), BF16), V((count, conv), BF16), V((EXTRA, conv), BF16), V((count + EXTRA, conv), F32),
        V((count, conv), BF16), V((count, mem), BF16),
        V((8, count), F32), V((n_tp, 8, count), F32),
        V((count, model), BF16), V((n_tp, share, model), BF16),
        S((9,)), S, S((n_tp,)), S((n_tp,)),
        S((heads, NCHUNK + 1)), S((heads, NCHUNK + 1)), S((heads, NCHUNK + 1)), S((heads, NCHUNK + 1)),
        S, S, S((n_tp,)), S((n_tp,)), S((NOUT, n_tp)), S((NOUT, n_tp)),
    ]
    return pl.pallas_call(
        functools.partial(kernel, n_sp, n_tp, heads),
        out_shape=jax.ShapeDtypeStruct((share, model), BF16),
        in_specs=[hbm, vmem, hbm, hbm, hbm, vmem, hbm, hbm, hbm, hbm, vmem, vmem, vmem, hbm, hbm],
        out_specs=vmem,
        scratch_shapes=scratch,
        compiler_params=pltpu.CompilerParams(
            collective_id=0, has_side_effects=True, vmem_limit_bytes=60 * 1024 * 1024),
        name="mixer",
    )(tokens, norm_gain, conv_b_w, conv_c_w, conv_u_w, conv_taps, query_w, key_w, value_w, outgate_w,
      gates_w, gate_bias, mem_gain, conv_out_w, mem_out_w)


def solution(mesh):
    n_sp, n_tp = mesh.shape["sp"], mesh.shape["tp"]
    cols, rows = P(None, "tp"), P("tp", None)
    return jax.shard_map(
        functools.partial(body, n_sp, n_tp),
        mesh=mesh,
        in_specs=(
            P("sp", "tp"), cols, cols, cols, cols, cols, cols, cols, cols, cols,
            P(None, None, "tp"), cols, P("tp"), rows, rows,
        ),
        out_specs=P(("sp", "tp"), None),
        check_vma=False,
    )
```

```python
import functools

import jax
import jax.numpy as jnp
from jax import lax
from jax.experimental import pallas as pl
from jax.experimental.pallas import tpu as pltpu
from jax.sharding import PartitionSpec as P

EPS = 1e-06
LOWEST = -1e30
HIGH = lax.Precision.HIGHEST
MESH = pl.DeviceIdType.MESH
F32 = jnp.float32
BF16 = jnp.bfloat16
GROUP = 128
NCHUNK = 4
NOUT = 4
EXTRA = 16


def dot(a, b, dims=((1,), (0,)), precision=None):
    return lax.dot_general(a, b, (dims, ((), ())), precision=precision, preferred_element_type=F32)


def kernel(n_sp, n_tp, heads, *refs):
    (tok, gain, wb, wc, wu, taps, wq, wk, wv, wo, gw, bias, mgain, cow, mow, out) = refs[:16]
    (
        full, scaled, vb, vc, vu, vq, vk, vv, vo, vg, raw_g, raw_b, vco, vmo,
        qs, ks, vs, og, own_c, got_a, got_p, put_p, in_c,
        meta, meta_a, meta_p, meta_s, meta_i, gates, gates_t,
        num, den, gb, mixed, halo, pad, yc, ym, sq_own, sq_got, part, rs, acc_c, acc_m, from_mate, summed,
        sem_w, sem_tok, tok_s, tok_r, a_s, a_r, p_s, p_r, h_s, h_r, q_s, q_r, r_s, r_r, d_s, d_r,
    ) = refs[16:]
    sp, tp = lax.axis_index("sp"), lax.axis_index("tp")
    count, feats = tok.shape
    model = n_tp * feats
    head_dim = wq.shape[1] // heads
    rows = head_dim // NCHUNK
    chips = n_tp // 2
    chip, core = tp // 2, lax.rem(tp, 2)
    mate = chip * 2 + 1 - core
    pair, odd = sp // 2, lax.rem(sp, 2)
    last_pair = n_sp // 2 - 1
    twin = sp + 1 - 2 * odd
    others = [lax.rem(tp + k, n_tp) for k in range(1, n_tp)]

    tok_copy = pltpu.make_async_copy(tok, full.at[tp, pl.ds(0, count)], sem_tok)
    tok_copy.start()
    loads = [
        pltpu.make_async_copy(src, dst, sem_w.at[i])
        for i, (src, dst) in enumerate(
            ((wk, vk), (wv, vv), (wq, vq), (wc, vc), (wu, vu), (wb, vb), (wo, vo), (cow, vco), (mow, vmo))
        )
    ]
    for load in loads:
        load.start()
    wait_of = dict(zip(("k", "v", "q", "c", "u", "b", "o", "co", "mo"), loads))
    full[tp, pl.ds(count, EXTRA), :] = jnp.broadcast_to(gain[...].astype(F32), (EXTRA, feats)).astype(BF16)

    raw_g[...] = jnp.zeros(raw_g.shape, F32)
    raw_b[...] = jnp.zeros(raw_b.shape, F32)
    for i in range(2):
        raw_g[i * heads:(i + 1) * heads, :] = gw[i].astype(F32)
        raw_b[0:1, i * heads:(i + 1) * heads] = bias[i:i + 1, :]
    vg[0:EXTRA, :] = raw_g[...].astype(BF16)
    vg[EXTRA:GROUP, :] = jnp.zeros((GROUP - EXTRA, model), BF16)

    barrier = pltpu.get_barrier_semaphore()
    steps = (1, -1, 2, -2)
    for other in others:
        pl.semaphore_signal(barrier, inc=1, device_id=(sp, other), device_id_type=MESH)
    for step in steps:
        @pl.when((sp + step >= 0) & (sp + step < n_sp))
        def _():
            pl.semaphore_signal(barrier, inc=1, device_id=(sp + step, tp), device_id_type=MESH)
    peers = n_tp - 1
    for step in steps:
        peers = peers + ((sp + step >= 0) & (sp + step < n_sp)).astype(jnp.int32)
    pl.semaphore_wait(barrier, peers)

    def send_tok(source, to, slot):
        copy = pltpu.make_async_remote_copy(
            src_ref=full.at[source], dst_ref=full.at[source], send_sem=tok_s.at[slot],
            recv_sem=tok_r.at[source], device_id=(sp, to), device_id_type=MESH)
        copy.start()
        return copy

    def got_tok(source):
        pltpu.make_async_remote_copy(
            src_ref=full.at[source], dst_ref=full.at[source], send_sem=tok_s.at[0],
            recv_sem=tok_r.at[source], device_id=(sp, mate), device_id_type=MESH).wait_recv()

    tok_copy.wait()
    tok_sends = []
    far = [lax.rem(chip + k, chips) for k in range(1, chips)]
    for k, x in enumerate(far):
        tok_sends.append(send_tok(tp, x * 2 + core, k))
    tok_sends.append(send_tok(tp, mate, chips - 1))
    def take(source):
        wide = full[source, 0:count, :].astype(F32)
        gains = full[source, count:count + 1, :].astype(F32)
        scaled[:, pl.ds(pl.multiple_of(source * feats, GROUP), feats)] = (wide * gains).astype(BF16)
        return jnp.sum(wide * wide, axis=1, keepdims=True)

    squares = take(tp)
    got_tok(mate)
    squares = squares + take(mate)
    for k, x in enumerate(far):
        got_tok(x * 2 + core)
        tok_sends.append(send_tok(x * 2 + core, mate, chips + k))
        squares = squares + take(x * 2 + core)
    for k, x in enumerate(far):
        got_tok(x * 2 + 1 - core)
        squares = squares + take(x * 2 + 1 - core)
    inv = lax.rsqrt(squares / model + EPS)

    def project(ref, lo, hi):
        return (inv * dot(scaled[...], ref[:, lo:hi])).astype(BF16)

    pre = inv * dot(scaled[...], vg[...], ((1,), (1,))) + raw_b[0:1, :]
    lf = jnp.minimum(pre, 0.0) - jnp.log1p(jnp.exp(-jnp.abs(pre)))
    row_id = lax.broadcasted_iota(jnp.int32, (count, count), 0)
    col_id = lax.broadcasted_iota(jnp.int32, (count, count), 1)
    causal = row_id >= col_id
    running = dot(causal.astype(F32), lf, precision=HIGH)
    lane = lax.broadcasted_iota(jnp.int32, (count, GROUP), 1)
    both = jnp.where(lane < heads, pre, running)
    gates[...] = both
    gates_t[...] = both.T

    def gate_parts(h):
        i_col, b_col = gates[:, h:h + 1], gates[:, heads + h:heads + h + 1]
        i_row, b_row = gates_t[h:h + 1, :], gates_t[heads + h:heads + h + 1, :]
        decays = jnp.where(causal, b_col - b_row + i_row, LOWEST)
        top = jnp.max(decays, axis=1, keepdims=True)
        return i_col, b_col, decays, top

    wait_of["k"].wait()
    wait_of["v"].wait()
    scale = head_dim ** -0.5
    a_sends = []

    def remote(src, dst, ss, rs_, to):
        return pltpu.make_async_remote_copy(
            src_ref=src, dst_ref=dst, send_sem=ss, recv_sem=rs_, device_id=to, device_id_type=MESH)

    for h in range(heads):
        lo, hi = h * head_dim, (h + 1) * head_dim
        ks[:, lo:hi] = project(vk, lo, hi)
        vs[:, lo:hi] = project(vv, lo, hi)
        i_col, b_col, _, top = gate_parts(h)
        total = b_col[count - 1:count, :]
        m_own = top[count - 1:count, :]
        weight = jnp.exp(total - b_col + i_col - m_own)
        wkeys = ks[:, lo:hi].astype(F32) * (weight * scale)
        meta[h, 0:1, :] = jnp.sum(wkeys, axis=0, keepdims=True)
        meta[h, 1:2, :] = jnp.broadcast_to(m_own, (1, head_dim))
        meta[h, 2:3, :] = jnp.broadcast_to(total, (1, head_dim))
        meta[h, 3:8, :] = jnp.zeros((5, head_dim), F32)
        own_c[h] = dot(wkeys.astype(BF16), vs[:, lo:hi], ((0,), (0,))).astype(BF16)
        copy = remote(meta.at[h], meta_a.at[h], a_s.at[h, NCHUNK], a_r.at[h, NCHUNK], (twin, tp))
        copy.start()
        a_sends.append(copy)
        for c in range(NCHUNK):
            at = pl.ds(c * rows, rows)
            copy = remote(own_c.at[h, at], got_a.at[h, at], a_s.at[h, c], a_r.at[h, c], (twin, tp))
            copy.start()
            a_sends.append(copy)

    wait_of["c"].wait()
    wait_of["u"].wait()
    conv = wc.shape[1]
    mix = (project(vc, 0, conv).astype(F32) * project(vu, 0, conv).astype(F32)).astype(BF16)
    mixed[...] = mix
    edge = remote(mixed.at[pl.ds(count - EXTRA, EXTRA)], halo, h_s, h_r, (sp + 1, tp))
    pl.when(sp < n_sp - 1)(edge.start)
    wait_of["q"].wait()
    for h in range(heads):
        qs[:, h * head_dim:(h + 1) * head_dim] = project(vq, h * head_dim, (h + 1) * head_dim)
    wait_of["b"].wait()
    gb[...] = project(vb, 0, conv)
    wait_of["o"].wait()
    for h in range(heads):
        og[:, h * head_dim:(h + 1) * head_dim] = project(vo, h * head_dim, (h + 1) * head_dim)

    def local_part():
        for h in range(heads):
            lo, hi = h * head_dim, (h + 1) * head_dim
            _, _, decays, top = gate_parts(h)
            scores = dot(qs[:, lo:hi], ks[:, lo:hi], ((1,), (1,))) * scale * jnp.exp(decays - top)
            den[h] = jnp.broadcast_to(jnp.sum(scores, axis=1, keepdims=True), (count, GROUP))
            num[h] = dot(scores.astype(BF16), vs[:, lo:hi])

        @pl.when(sp > 0)
        def _():
            edge.wait_recv()

        @pl.when(sp == 0)
        def _():
            halo[...] = jnp.zeros(halo.shape, BF16)
        pad[0:EXTRA, :] = halo[...].astype(F32)
        pad[EXTRA:EXTRA + count, :] = mixed[...].astype(F32)
        reach = taps.shape[0] - 1
        tap = taps[...].astype(F32)
        acc = tap[0:1, :] * pad[EXTRA - reach:EXTRA - reach + count, :]
        for j in range(1, reach + 1):
            acc = acc + tap[j:j + 1, :] * pad[EXTRA - reach + j:EXTRA - reach + j + count, :]
        yc[...] = (gb[...].astype(F32) * acc).astype(BF16)

    early = pair >= (last_pair + 1) // 2
    pl.when(early)(local_part)

    is_odd = odd == 1

    @pl.when(pair == 0)
    def _():
        for h in range(heads):
            got_p[h] = jnp.zeros((head_dim, head_dim), BF16)
            meta_p[h] = jnp.full((8, head_dim), 0.0, F32)
            meta_p[h, 1:2, :] = jnp.full((1, head_dim), LOWEST, F32)

    def chain(h, c):
        at = pl.ds(c * rows, rows)
        if c == NCHUNK:
            return remote(meta_s.at[h], meta_p.at[h], p_s.at[h, c], p_r.at[h, c], (sp + 2, tp))
        return remote(put_p.at[h, at], got_p.at[h, at], p_s.at[h, c], p_r.at[h, c], (sp + 2, tp))

    def pair_copy(h, c):
        return a_sends[h * (NCHUNK + 1) + (0 if c == NCHUNK else c + 1)]

    for h in range(heads):
        pair_copy(h, NCHUNK).wait_recv()
        pl.when(pair > 0)(chain(h, NCHUNK).wait_recv)
        own, got, before = meta[h], meta_a[h], meta_p[h]
        first = jnp.where(is_odd, got, own)
        second = jnp.where(is_odd, own, got)
        m_p, m_e, m_o = before[1:2, :], first[1:2, :], second[1:2, :]
        b_e, b_o = first[2:3, :], second[2:3, :]
        m_1 = jnp.maximum(b_e + m_p, m_e)
        m_2 = jnp.maximum(b_o + m_1, m_o)
        c_p = jnp.exp(b_o + (b_e + m_p) - m_2)
        c_e = jnp.exp(b_o + m_e - m_2)
        c_o = jnp.exp(m_o - m_2)
        meta_s[h] = jnp.zeros((8, head_dim), F32)
        meta_s[h, 0:1, :] = c_p * before[0:1, :] + c_e * first[0:1, :] + c_o * second[0:1, :]
        meta_s[h, 1:2, :] = m_2
        pl.when(pair < last_pair)(chain(h, NCHUNK).start)
        c_own = jnp.where(is_odd, c_o, c_e)
        c_got = jnp.where(is_odd, c_e, c_o)
        f_p = jnp.where(is_odd, jnp.exp(b_e + m_p - m_1), 1.0)
        f_e = jnp.where(is_odd, jnp.exp(m_e - m_1), 0.0)
        meta_in = (f_p * before[0:1, :] + f_e * first[0:1, :], jnp.where(is_odd, m_1, m_p))
        meta_i[h, 0:1, :] = meta_in[0]
        meta_i[h, 1:2, :] = meta_in[1]
        for c in range(NCHUNK):
            at = pl.ds(c * rows, rows)
            pair_copy(h, c).wait_recv()
            pl.when(pair > 0)(chain(h, c).wait_recv)
            block_p = got_p[h, at, :].astype(F32)
            block_a = got_a[h, at, :].astype(F32)
            put_p[h, at, :] = (c_p * block_p + c_own * own_c[h, at, :].astype(F32) + c_got * block_a).astype(BF16)
            pl.when(pair < last_pair)(chain(h, c).start)
            in_c[h, at, :] = (f_p * block_p + f_e * block_a).astype(BF16)

    pl.when(jnp.logical_not(early))(local_part)

    own_sq = jnp.zeros((count, 1), F32)
    for h in range(heads):
        lo, hi = h * head_dim, (h + 1) * head_dim
        _, b_col, _, top_own = gate_parts(h)
        n_in, m_in = meta_i[h, 0:1, :], meta_i[h, 1:2, 0:1]
        top = jnp.maximum(top_own, b_col + m_in)
        s_own = jnp.exp(top_own - top)
        s_in = jnp.exp(b_col + m_in - top)
        qh = qs[:, lo:hi]
        den_all = s_own * den[h, :, 0:1] + s_in * jnp.sum(qh.astype(F32) * n_in, axis=1, keepdims=True)
        num_all = s_own * num[h] + s_in * dot(qh, in_c[h])
        raw = num_all / jnp.maximum(jnp.abs(den_all), jnp.exp(-top))
        own_sq = own_sq + jnp.sum(raw * raw, axis=1, keepdims=True)
        sig = 1.0 / (1.0 + jnp.exp(-og[:, lo:hi].astype(F32)))
        ym[:, lo:hi] = (sig * raw * mgain[lo:hi].astype(F32).reshape(1, head_dim)).astype(BF16)
    sq_own[...] = jnp.broadcast_to(own_sq, (count, GROUP)).T[0:8, :]
    sq_sends = []
    for k, other in enumerate(others):
        copy = remote(sq_own, sq_got.at[tp], q_s.at[k], q_r.at[tp], (sp, other))
        copy.start()
        sq_sends.append(copy)
    wait_of["co"].wait()
    wait_of["mo"].wait()
    share = count // n_tp
    width = model // NOUT
    for j in range(NOUT):
        lo, hi = j * width, (j + 1) * width
        acc_c[:, lo:hi] = dot(yc[...], vco[:, lo:hi])
        acc_m[:, lo:hi] = dot(ym[...], vmo[:, lo:hi])
    total_sq = sq_own[...]
    for k, other in enumerate(others):
        remote(sq_own, sq_got.at[other], q_s.at[k], q_r.at[other], (sp, other)).wait_recv()
        total_sq = total_sq + sq_got[other]
    features = n_tp * heads * head_dim
    norm_row = lax.rsqrt(total_sq[0:1, :] / features + EPS)
    norm = jnp.broadcast_to(norm_row, (count, count)).T[:, 0:1]
    def block(x, y):
        return pl.ds(pl.multiple_of((x * 2 + y) * share, share), share)

    def mate_copy(j, x):
        at = pl.ds(j * width, width)
        return remote(part.at[block(x, 1 - core), at], from_mate.at[x, :, at], d_s.at[j, x], d_r.at[j, x], (sp, mate))

    def far_copy(j, x):
        at = pl.ds(j * width, width)
        return remote(summed.at[x, :, at], rs.at[chip, :, at], r_s.at[j, x], r_r.at[j, chip], (sp, x * 2 + core))

    out_sends = []
    for j in range(NOUT):
        lo, hi = j * width, (j + 1) * width
        part[:, lo:hi] = (acc_c[:, lo:hi] + norm * acc_m[:, lo:hi]).astype(BF16)
        for x in far + [chip]:
            copy = mate_copy(j, x)
            copy.start()
            out_sends.append(copy)

    def both_cores(j, x):
        lo, hi = j * width, (j + 1) * width
        mate_copy(j, x).wait_recv()
        return part[block(x, core), lo:hi].astype(F32) + from_mate[x, :, lo:hi].astype(F32)

    for j in range(NOUT):
        for x in far:
            summed[x, :, j * width:(j + 1) * width] = both_cores(j, x).astype(BF16)
            copy = far_copy(j, x)
            copy.start()
            out_sends.append(copy)
    for j in range(NOUT):
        lo, hi = j * width, (j + 1) * width
        at = pl.ds(lo, width)
        acc = both_cores(j, chip)
        for x in far:
            remote(summed.at[x, :, at], rs.at[x, :, at], r_s.at[j, x], r_r.at[j, x], (sp, x * 2 + core)).wait_recv()
            acc = acc + rs[x, :, lo:hi].astype(F32)
        out[:, lo:hi] = acc.astype(BF16)

    for copy in tok_sends + a_sends + sq_sends + out_sends:
        copy.wait_send()
    pl.when(sp < n_sp - 1)(edge.wait_send)

    @pl.when(pair < last_pair)
    def _():
        for h in range(heads):
            for c in range(NCHUNK + 1):
                chain(h, c).wait_send()


def body(n_sp, n_tp, tokens, norm_gain, conv_b_w, conv_c_w, conv_u_w, conv_taps, query_w, key_w,
         value_w, outgate_w, gate_w, gate_bias, mem_gain, conv_out_w, mem_out_w):
    count, feats = tokens.shape
    model, conv = conv_b_w.shape
    mem = query_w.shape[1]
    heads = gate_bias.shape[1]
    head_dim = mem // heads
    share, chips = count // n_tp, n_tp // 2
    gates_w = jnp.transpose(gate_w, (1, 2, 0))
    vmem, hbm = pl.BlockSpec(memory_space=pltpu.VMEM), pl.BlockSpec(memory_space=pl.ANY)
    V, S = pltpu.VMEM, pltpu.SemaphoreType.DMA
    state = V((heads, head_dim, head_dim), BF16)
    small = V((heads, 8, head_dim), F32)
    scratch = [
        V((n_tp, count + EXTRA, feats), BF16), V((count, model), BF16),
        V((model, conv), BF16), V((model, conv), BF16), V((model, conv), BF16),
        V((model, mem), BF16), V((model, mem), BF16), V((model, mem), BF16), V((model, mem), BF16),
        V((GROUP, model), BF16), V((EXTRA, model), F32), V((8, GROUP), F32), V((conv, model), BF16), V((mem, model), BF16),
        V((count, mem), BF16), V((count, mem), BF16), V((count, mem), BF16), V((count, mem), BF16),
        state, state, state, state, state,
        small, small, small, small, small, V((count, GROUP), F32), V((GROUP, count), F32),
        V((heads, count, head_dim), F32), V((heads, count, GROUP), F32),
        V((count, conv), BF16), V((count, conv), BF16), V((EXTRA, conv), BF16), V((count + EXTRA, conv), F32),
        V((count, conv), BF16), V((count, mem), BF16),
        V((8, count), F32), V((n_tp, 8, count), F32),
        V((count, model), BF16), V((chips, share, model), BF16),
        V((count, model), F32), V((count, model), F32), V((chips, share, model), BF16), V((chips, share, model), BF16),
        S((9,)), S, S((n_tp,)), S((n_tp,)),
        S((heads, NCHUNK + 1)), S((heads, NCHUNK + 1)), S((heads, NCHUNK + 1)), S((heads, NCHUNK + 1)),
        S, S, S((n_tp,)), S((n_tp,)), S((NOUT, chips)), S((NOUT, chips)), S((NOUT, chips)), S((NOUT, chips)),
    ]
    return pl.pallas_call(
        functools.partial(kernel, n_sp, n_tp, heads),
        out_shape=jax.ShapeDtypeStruct((share, model), BF16),
        in_specs=[hbm, vmem, hbm, hbm, hbm, vmem, hbm, hbm, hbm, hbm, vmem, vmem, vmem, hbm, hbm],
        out_specs=vmem,
        scratch_shapes=scratch,
        compiler_params=pltpu.CompilerParams(
            collective_id=0, has_side_effects=True, vmem_limit_bytes=60 * 1024 * 1024),
        name="mixer",
    )(tokens, norm_gain, conv_b_w, conv_c_w, conv_u_w, conv_taps, query_w, key_w, value_w, outgate_w,
      gates_w, gate_bias, mem_gain, conv_out_w, mem_out_w)


def solution(mesh):
    n_sp, n_tp = mesh.shape["sp"], mesh.shape["tp"]
    cols, rows = P(None, "tp"), P("tp", None)
    return jax.shard_map(
        functools.partial(body, n_sp, n_tp),
        mesh=mesh,
        in_specs=(
            P("sp", "tp"), cols, cols, cols, cols, cols, cols, cols, cols, cols,
            P(None, None, "tp"), cols, P("tp"), rows, rows,
        ),
        out_specs=P(("sp", "tp"), None),
        check_vma=False,
    )
```

```python
import functools

import jax
import jax.numpy as jnp
from jax import lax
from jax.experimental import pallas as pl
from jax.experimental.pallas import tpu as pltpu
from jax.sharding import PartitionSpec as P

EPS = 1e-06
LOWEST = -1e30
HIGH = lax.Precision.HIGHEST
MESH = pl.DeviceIdType.MESH
F32 = jnp.float32
BF16 = jnp.bfloat16
GROUP = 128
NCHUNK = 8
NOUT = 2
EXTRA = 16


def dot(a, b, dims=((1,), (0,)), precision=None):
    return lax.dot_general(a, b, (dims, ((), ())), precision=precision, preferred_element_type=F32)


def kernel(n_sp, n_tp, heads, *refs):
    (tok, gain, wb, wc, wu, taps, wq, wk, wv, wo, gw, bias, mgain, cow, mow, out) = refs[:16]
    (
        full, scaled, vb, vc, vu, vq, vk, vv, vo, vg, raw_g, raw_b, vco, vmo,
        qs, ks, vs, og, own_c, got_a, got_p, put_p, in_c,
        meta, meta_a, meta_p, meta_s, meta_i, gates, gates_t,
        num, den, gb, mixed, halo, pad, yc, ym, sq_own, sq_got, part, rs, acc_c, acc_m, from_mate, summed,
        sem_w, sem_tok, tok_s, tok_r, a_s, a_r, p_s, p_r, h_s, h_r, q_s, q_r, r_s, r_r, d_s, d_r,
    ) = refs[16:]
    sp, tp = lax.axis_index("sp"), lax.axis_index("tp")
    count, feats = tok.shape
    model = n_tp * feats
    head_dim = wq.shape[1] // heads
    rows = head_dim // NCHUNK
    chips = n_tp // 2
    chip, core = tp // 2, lax.rem(tp, 2)
    mate = chip * 2 + 1 - core
    pair, odd = sp // 2, lax.rem(sp, 2)
    last_pair = n_sp // 2 - 1
    twin = sp + 1 - 2 * odd
    others = [lax.rem(tp + k, n_tp) for k in range(1, n_tp)]

    tok_copy = pltpu.make_async_copy(tok, full.at[tp, pl.ds(0, count)], sem_tok)
    tok_copy.start()
    loads = [
        pltpu.make_async_copy(src, dst, sem_w.at[i])
        for i, (src, dst) in enumerate(
            ((wk, vk), (wv, vv), (wq, vq), (wc, vc), (wu, vu), (wb, vb), (wo, vo), (cow, vco), (mow, vmo))
        )
    ]
    for load in loads:
        load.start()
    wait_of = dict(zip(("k", "v", "q", "c", "u", "b", "o", "co", "mo"), loads))
    full[tp, pl.ds(count, EXTRA), :] = jnp.broadcast_to(gain[...].astype(F32), (EXTRA, feats)).astype(BF16)

    raw_g[...] = jnp.zeros(raw_g.shape, F32)
    raw_b[...] = jnp.zeros(raw_b.shape, F32)
    for i in range(2):
        raw_g[i * heads:(i + 1) * heads, :] = gw[i].astype(F32)
        raw_b[0:1, i * heads:(i + 1) * heads] = bias[i:i + 1, :]
    vg[0:EXTRA, :] = raw_g[...].astype(BF16)
    vg[EXTRA:GROUP, :] = jnp.zeros((GROUP - EXTRA, model), BF16)

    barrier = pltpu.get_barrier_semaphore()
    steps = (1, -1, 2, -2)
    for other in others:
        pl.semaphore_signal(barrier, inc=1, device_id=(sp, other), device_id_type=MESH)
    for step in steps:
        @pl.when((sp + step >= 0) & (sp + step < n_sp))
        def _():
            pl.semaphore_signal(barrier, inc=1, device_id=(sp + step, tp), device_id_type=MESH)
    peers = n_tp - 1
    for step in steps:
        peers = peers + ((sp + step >= 0) & (sp + step < n_sp)).astype(jnp.int32)
    pl.semaphore_wait(barrier, peers)

    def send_tok(source, to, slot):
        copy = pltpu.make_async_remote_copy(
            src_ref=full.at[source], dst_ref=full.at[source], send_sem=tok_s.at[slot],
            recv_sem=tok_r.at[source], device_id=(sp, to), device_id_type=MESH)
        copy.start()
        return copy

    def got_tok(source):
        pltpu.make_async_remote_copy(
            src_ref=full.at[source], dst_ref=full.at[source], send_sem=tok_s.at[0],
            recv_sem=tok_r.at[source], device_id=(sp, mate), device_id_type=MESH).wait_recv()

    tok_copy.wait()
    tok_sends = []
    far = [lax.rem(chip + k, chips) for k in range(1, chips)]
    for k, x in enumerate(far):
        tok_sends.append(send_tok(tp, x * 2 + core, k))
    tok_sends.append(send_tok(tp, mate, chips - 1))
    mem = wk.shape[1]
    wait_of["k"].wait()
    wait_of["v"].wait()

    def take(source, first=False):
        wide = full[source, 0:count, :].astype(F32)
        gains = full[source, count:count + 1, :].astype(F32)
        piece = (wide * gains).astype(BF16)
        at = pl.ds(pl.multiple_of(source * feats, GROUP), feats)
        scaled[:, at] = piece
        for lo, hi, update in (
            (2 * mem, 2 * mem + GROUP, dot(piece, vg[:, at], ((1,), (1,)))),
            (0, mem, dot(piece, vk[at, :])),
            (mem, 2 * mem, dot(piece, vv[at, :])),
        ):
            acc_c[:, lo:hi] = update if first else acc_c[:, lo:hi] + update
        return jnp.sum(wide * wide, axis=1, keepdims=True)

    squares = take(tp, True)
    got_tok(mate)
    squares = squares + take(mate)
    for k, x in enumerate(far):
        got_tok(x * 2 + core)
        tok_sends.append(send_tok(x * 2 + core, mate, chips + k))
        squares = squares + take(x * 2 + core)
    for k, x in enumerate(far):
        got_tok(x * 2 + 1 - core)
        squares = squares + take(x * 2 + 1 - core)
    inv = lax.rsqrt(squares / model + EPS)

    def project(ref, lo, hi):
        return (inv * dot(scaled[...], ref[:, lo:hi])).astype(BF16)

    pre = inv * acc_c[:, 2 * mem:2 * mem + GROUP] + raw_b[0:1, :]
    lf = jnp.minimum(pre, 0.0) - jnp.log1p(jnp.exp(-jnp.abs(pre)))
    row_id = lax.broadcasted_iota(jnp.int32, (count, count), 0)
    col_id = lax.broadcasted_iota(jnp.int32, (count, count), 1)
    causal = row_id >= col_id
    running = dot(causal.astype(F32), lf, precision=HIGH)
    lane = lax.broadcasted_iota(jnp.int32, (count, GROUP), 1)
    both = jnp.where(lane < heads, pre, running)
    gates[...] = both
    gates_t[...] = both.T

    def gate_parts(h):
        i_col, b_col = gates[:, h:h + 1], gates[:, heads + h:heads + h + 1]
        i_row, b_row = gates_t[h:h + 1, :], gates_t[heads + h:heads + h + 1, :]
        decays = jnp.where(causal, b_col - b_row + i_row, LOWEST)
        top = jnp.max(decays, axis=1, keepdims=True)
        return i_col, b_col, decays, top

    scale = head_dim ** -0.5
    a_sends = []

    def remote(src, dst, ss, rs_, to):
        return pltpu.make_async_remote_copy(
            src_ref=src, dst_ref=dst, send_sem=ss, recv_sem=rs_, device_id=to, device_id_type=MESH)

    for h in range(heads):
        lo, hi = h * head_dim, (h + 1) * head_dim
        ks[:, lo:hi] = (inv * acc_c[:, lo:hi]).astype(BF16)
        vs[:, lo:hi] = (inv * acc_c[:, mem + lo:mem + hi]).astype(BF16)
        i_col, b_col, _, top = gate_parts(h)
        total = b_col[count - 1:count, :]
        m_own = top[count - 1:count, :]
        weight = jnp.exp(total - b_col + i_col - m_own)
        wkeys = ks[:, lo:hi].astype(F32) * (weight * scale)
        meta[h, 0:1, :] = jnp.sum(wkeys, axis=0, keepdims=True)
        meta[h, 1:2, :] = jnp.broadcast_to(m_own, (1, head_dim))
        meta[h, 2:3, :] = jnp.broadcast_to(total, (1, head_dim))
        meta[h, 3:8, :] = jnp.zeros((5, head_dim), F32)
        own_c[h] = dot(wkeys.astype(BF16), vs[:, lo:hi], ((0,), (0,))).astype(BF16)
        copy = remote(meta.at[h], meta_a.at[h], a_s.at[h, NCHUNK], a_r.at[h, NCHUNK], (twin, tp))
        copy.start()
        a_sends.append(copy)
        for c in range(NCHUNK):
            at = pl.ds(c * rows, rows)
            copy = remote(own_c.at[h, at], got_a.at[h, at], a_s.at[h, c], a_r.at[h, c], (twin, tp))
            copy.start()
            a_sends.append(copy)

    wait_of["c"].wait()
    wait_of["u"].wait()
    conv = wc.shape[1]
    mix = (project(vc, 0, conv).astype(F32) * project(vu, 0, conv).astype(F32)).astype(BF16)
    mixed[...] = mix
    edge = remote(mixed.at[pl.ds(count - EXTRA, EXTRA)], halo, h_s, h_r, (sp + 1, tp))
    pl.when(sp < n_sp - 1)(edge.start)

    wait_of["b"].wait()
    wait_of["o"].wait()
    wait_of["q"].wait()

    def local_part():
        for h in range(heads):
            qs[:, h * head_dim:(h + 1) * head_dim] = project(vq, h * head_dim, (h + 1) * head_dim)
        gb[...] = project(vb, 0, conv)
        for h in range(heads):
            og[:, h * head_dim:(h + 1) * head_dim] = project(vo, h * head_dim, (h + 1) * head_dim)
        for h in range(heads):
            lo, hi = h * head_dim, (h + 1) * head_dim
            _, _, decays, top = gate_parts(h)
            scores = dot(qs[:, lo:hi], ks[:, lo:hi], ((1,), (1,))) * scale * jnp.exp(decays - top)
            den[h] = jnp.broadcast_to(jnp.sum(scores, axis=1, keepdims=True), (count, GROUP))
            num[h] = dot(scores.astype(BF16), vs[:, lo:hi])


    early = pair >= (last_pair + 1) // 2
    pl.when(early)(local_part)

    is_odd = odd == 1

    @pl.when(pair == 0)
    def _():
        for h in range(heads):
            got_p[h] = jnp.zeros((head_dim, head_dim), BF16)
            meta_p[h] = jnp.full((8, head_dim), 0.0, F32)
            meta_p[h, 1:2, :] = jnp.full((1, head_dim), LOWEST, F32)

    def chain(h, c):
        at = pl.ds(c * rows, rows)
        if c == NCHUNK:
            return remote(meta_s.at[h], meta_p.at[h], p_s.at[h, c], p_r.at[h, c], (sp + 2, tp))
        return remote(put_p.at[h, at], got_p.at[h, at], p_s.at[h, c], p_r.at[h, c], (sp + 2, tp))

    def pair_copy(h, c):
        return a_sends[h * (NCHUNK + 1) + (0 if c == NCHUNK else c + 1)]

    for h in range(heads):
        pair_copy(h, NCHUNK).wait_recv()
        pl.when(pair > 0)(chain(h, NCHUNK).wait_recv)
        own, got, before = meta[h], meta_a[h], meta_p[h]
        first = jnp.where(is_odd, got, own)
        second = jnp.where(is_odd, own, got)
        m_p, m_e, m_o = before[1:2, :], first[1:2, :], second[1:2, :]
        b_e, b_o = first[2:3, :], second[2:3, :]
        m_1 = jnp.maximum(b_e + m_p, m_e)
        m_2 = jnp.maximum(b_o + m_1, m_o)
        c_p = jnp.exp(b_o + (b_e + m_p) - m_2)
        c_e = jnp.exp(b_o + m_e - m_2)
        c_o = jnp.exp(m_o - m_2)
        meta_s[h] = jnp.zeros((8, head_dim), F32)
        meta_s[h, 0:1, :] = c_p * before[0:1, :] + c_e * first[0:1, :] + c_o * second[0:1, :]
        meta_s[h, 1:2, :] = m_2
        pl.when(pair < last_pair)(chain(h, NCHUNK).start)
        c_own = jnp.where(is_odd, c_o, c_e)
        c_got = jnp.where(is_odd, c_e, c_o)
        f_p = jnp.where(is_odd, jnp.exp(b_e + m_p - m_1), 1.0)
        f_e = jnp.where(is_odd, jnp.exp(m_e - m_1), 0.0)
        meta_in = (f_p * before[0:1, :] + f_e * first[0:1, :], jnp.where(is_odd, m_1, m_p))
        meta_i[h, 0:1, :] = meta_in[0]
        meta_i[h, 1:2, :] = meta_in[1]
        for c in range(NCHUNK):
            at = pl.ds(c * rows, rows)
            pair_copy(h, c).wait_recv()
            pl.when(pair > 0)(chain(h, c).wait_recv)
            block_p = got_p[h, at, :].astype(F32)
            block_a = got_a[h, at, :].astype(F32)
            put_p[h, at, :] = (c_p * block_p + c_own * own_c[h, at, :].astype(F32) + c_got * block_a).astype(BF16)
            pl.when(pair < last_pair)(chain(h, c).start)
            in_c[h, at, :] = (f_p * block_p + f_e * block_a).astype(BF16)

    pl.when(jnp.logical_not(early))(local_part)

    @pl.when(sp > 0)
    def _():
        edge.wait_recv()

    @pl.when(sp == 0)
    def _():
        halo[...] = jnp.zeros(halo.shape, BF16)
    pad[0:EXTRA, :] = halo[...].astype(F32)
    pad[EXTRA:EXTRA + count, :] = mixed[...].astype(F32)
    reach = taps.shape[0] - 1
    tap = taps[...].astype(F32)
    acc = tap[0:1, :] * pad[EXTRA - reach:EXTRA - reach + count, :]
    for j in range(1, reach + 1):
        acc = acc + tap[j:j + 1, :] * pad[EXTRA - reach + j:EXTRA - reach + j + count, :]
    yc[...] = (gb[...].astype(F32) * acc).astype(BF16)


    own_sq = jnp.zeros((count, 1), F32)
    for h in range(heads):
        lo, hi = h * head_dim, (h + 1) * head_dim
        _, b_col, _, top_own = gate_parts(h)
        n_in, m_in = meta_i[h, 0:1, :], meta_i[h, 1:2, 0:1]
        top = jnp.maximum(top_own, b_col + m_in)
        s_own = jnp.exp(top_own - top)
        s_in = jnp.exp(b_col + m_in - top)
        qh = qs[:, lo:hi]
        den_all = s_own * den[h, :, 0:1] + s_in * jnp.sum(qh.astype(F32) * n_in, axis=1, keepdims=True)
        num_all = s_own * num[h] + s_in * dot(qh, in_c[h])
        raw = num_all / jnp.maximum(jnp.abs(den_all), jnp.exp(-top))
        own_sq = own_sq + jnp.sum(raw * raw, axis=1, keepdims=True)
        sig = 1.0 / (1.0 + jnp.exp(-og[:, lo:hi].astype(F32)))
        ym[:, lo:hi] = (sig * raw * mgain[lo:hi].astype(F32).reshape(1, head_dim)).astype(BF16)
    sq_own[...] = jnp.broadcast_to(own_sq, (count, GROUP)).T[0:8, :]
    sq_sends = []
    for k, other in enumerate(others):
        copy = remote(sq_own, sq_got.at[tp], q_s.at[k], q_r.at[tp], (sp, other))
        copy.start()
        sq_sends.append(copy)
    wait_of["co"].wait()
    wait_of["mo"].wait()
    share = count // n_tp
    width = model // NOUT
    for j in range(NOUT):
        lo, hi = j * width, (j + 1) * width
        acc_c[:, lo:hi] = dot(yc[...], vco[:, lo:hi])
        acc_m[:, lo:hi] = dot(ym[...], vmo[:, lo:hi])
    total_sq = sq_own[...]
    for k, other in enumerate(others):
        remote(sq_own, sq_got.at[other], q_s.at[k], q_r.at[other], (sp, other)).wait_recv()
        total_sq = total_sq + sq_got[other]
    features = n_tp * heads * head_dim
    norm_row = lax.rsqrt(total_sq[0:1, :] / features + EPS)
    norm = jnp.broadcast_to(norm_row, (count, count)).T[:, 0:1]
    def block(x, y):
        return pl.ds(pl.multiple_of((x * 2 + y) * share, share), share)

    def mate_copy(j, x):
        at = pl.ds(j * width, width)
        return remote(part.at[block(x, 1 - core), at], from_mate.at[x, :, at], d_s.at[j, x], d_r.at[j, x], (sp, mate))

    def far_copy(j, x):
        at = pl.ds(j * width, width)
        return remote(summed.at[x, :, at], rs.at[chip, :, at], r_s.at[j, x], r_r.at[j, chip], (sp, x * 2 + core))

    out_sends = []
    for j in range(NOUT):
        lo, hi = j * width, (j + 1) * width
        part[:, lo:hi] = (acc_c[:, lo:hi] + norm * acc_m[:, lo:hi]).astype(BF16)
        for x in far + [chip]:
            copy = mate_copy(j, x)
            copy.start()
            out_sends.append(copy)

    def both_cores(j, x):
        lo, hi = j * width, (j + 1) * width
        mate_copy(j, x).wait_recv()
        return part[block(x, core), lo:hi].astype(F32) + from_mate[x, :, lo:hi].astype(F32)

    for j in range(NOUT):
        for x in far:
            summed[x, :, j * width:(j + 1) * width] = both_cores(j, x).astype(BF16)
            copy = far_copy(j, x)
            copy.start()
            out_sends.append(copy)
    for j in range(NOUT):
        lo, hi = j * width, (j + 1) * width
        at = pl.ds(lo, width)
        acc = both_cores(j, chip)
        for x in far:
            remote(summed.at[x, :, at], rs.at[x, :, at], r_s.at[j, x], r_r.at[j, x], (sp, x * 2 + core)).wait_recv()
            acc = acc + rs[x, :, lo:hi].astype(F32)
        out[:, lo:hi] = acc.astype(BF16)

    for copy in tok_sends + a_sends + sq_sends + out_sends:
        copy.wait_send()
    pl.when(sp < n_sp - 1)(edge.wait_send)

    @pl.when(pair < last_pair)
    def _():
        for h in range(heads):
            for c in range(NCHUNK + 1):
                chain(h, c).wait_send()


def body(n_sp, n_tp, tokens, norm_gain, conv_b_w, conv_c_w, conv_u_w, conv_taps, query_w, key_w,
         value_w, outgate_w, gate_w, gate_bias, mem_gain, conv_out_w, mem_out_w):
    count, feats = tokens.shape
    model, conv = conv_b_w.shape
    mem = query_w.shape[1]
    heads = gate_bias.shape[1]
    head_dim = mem // heads
    share, chips = count // n_tp, n_tp // 2
    gates_w = jnp.transpose(gate_w, (1, 2, 0))
    vmem, hbm = pl.BlockSpec(memory_space=pltpu.VMEM), pl.BlockSpec(memory_space=pl.ANY)
    V, S = pltpu.VMEM, pltpu.SemaphoreType.DMA
    state = V((heads, head_dim, head_dim), BF16)
    small = V((heads, 8, head_dim), F32)
    scratch = [
        V((n_tp, count + EXTRA, feats), BF16), V((count, model), BF16),
        V((model, conv), BF16), V((model, conv), BF16), V((model, conv), BF16),
        V((model, mem), BF16), V((model, mem), BF16), V((model, mem), BF16), V((model, mem), BF16),
        V((GROUP, model), BF16), V((EXTRA, model), F32), V((8, GROUP), F32), V((conv, model), BF16), V((mem, model), BF16),
        V((count, mem), BF16), V((count, mem), BF16), V((count, mem), BF16), V((count, mem), BF16),
        state, state, state, state, state,
        small, small, small, small, small, V((count, GROUP), F32), V((GROUP, count), F32),
        V((heads, count, head_dim), F32), V((heads, count, GROUP), F32),
        V((count, conv), BF16), V((count, conv), BF16), V((EXTRA, conv), BF16), V((count + EXTRA, conv), F32),
        V((count, conv), BF16), V((count, mem), BF16),
        V((8, count), F32), V((n_tp, 8, count), F32),
        V((count, model), BF16), V((chips, share, model), BF16),
        V((count, model), F32), V((count, model), F32), V((chips, share, model), BF16), V((chips, share, model), BF16),
        S((9,)), S, S((n_tp,)), S((n_tp,)),
        S((heads, NCHUNK + 1)), S((heads, NCHUNK + 1)), S((heads, NCHUNK + 1)), S((heads, NCHUNK + 1)),
        S, S, S((n_tp,)), S((n_tp,)), S((NOUT, chips)), S((NOUT, chips)), S((NOUT, chips)), S((NOUT, chips)),
    ]
    return pl.pallas_call(
        functools.partial(kernel, n_sp, n_tp, heads),
        out_shape=jax.ShapeDtypeStruct((share, model), BF16),
        in_specs=[hbm, vmem, hbm, hbm, hbm, vmem, hbm, hbm, hbm, hbm, vmem, vmem, vmem, hbm, hbm],
        out_specs=vmem,
        scratch_shapes=scratch,
        compiler_params=pltpu.CompilerParams(
            collective_id=0, has_side_effects=True, vmem_limit_bytes=60 * 1024 * 1024),
        name="mixer",
    )(tokens, norm_gain, conv_b_w, conv_c_w, conv_u_w, conv_taps, query_w, key_w, value_w, outgate_w,
      gates_w, gate_bias, mem_gain, conv_out_w, mem_out_w)


def solution(mesh):
    n_sp, n_tp = mesh.shape["sp"], mesh.shape["tp"]
    cols, rows = P(None, "tp"), P("tp", None)
    return jax.shard_map(
        functools.partial(body, n_sp, n_tp),
        mesh=mesh,
        in_specs=(
            P("sp", "tp"), cols, cols, cols, cols, cols, cols, cols, cols, cols,
            P(None, None, "tp"), cols, P("tp"), rows, rows,
        ),
        out_specs=P(("sp", "tp"), None),
        check_vma=False,
    )
```
